32 devices in a mesh: sp: 8 (over z, y), tp: 4 (over x, core).
Axes of the slice: x: 2, y: 2, z: 4, core: 2. Of those that a mesh axis runs over, the one named last changes fastest.
Arguments:
- hidden_state: bfloat16 [1024, 2048], P('sp'), may hold values from -6 to 6
- out_grad: bfloat16 [1024, 2048], P('sp'), may hold values from -8 to 8
- routes: int32 [1024, 2], P('sp'), may hold values from 0 to 3, all different within a row; in each aligned block of 128 rows (0 to 127, 128 to 255, ...) at most 96 rows name the same one
- route_weights: float32 [1024, 2], P('sp'), may hold values from 0.25 to 1
- w_gate: bfloat16 [8, 2048, 1792], P('sp', None, 'tp'), may hold values from -0.125 to 0.125
- w_up: bfloat16 [8, 2048, 1792], P('sp', None, 'tp'), may hold values from -0.125 to 0.125
- w_down: bfloat16 [8, 1792, 2048], P('sp', 'tp'), may hold values from -0.09375 to 0.09375
- value: bfloat16 [1024, 512], P('sp', 'tp'), may hold values from -6 to 6
- gate_in: bfloat16 [1024, 512], P('sp', 'tp'), may hold values from -6 to 6
- normed: bfloat16 [1024, 512], P('sp', 'tp'), may hold values from -24 to 24
- inv_std: float32 [1024], P('sp'), may hold values from 0.5 to 2
- norm_gain: float32 [512], P('tp'), may hold values from 0.1 to 1.9
- taps: float32 [31, 512], P(None, 'tp'), may hold values from -1 to 1
- w_proj: bfloat16 [2048, 512], P(None, 'tp'), may hold values from -0.25 to 0.25
Outputs:
- w_gate_grad: bfloat16 [8, 2048, 1792], P('sp', None, 'tp')
- w_up_grad: bfloat16 [8, 2048, 1792], P('sp', None, 'tp')
- w_down_grad: bfloat16 [8, 1792, 2048], P('sp', 'tp')
- stream_grad: bfloat16 [1024, 2048], P('sp', 'tp')
- proj_grad: float32 [2048, 512], P('sp', 'tp')
- value_grad: bfloat16 [1024, 512], P('sp', 'tp')
- gate_in_grad: bfloat16 [1024, 512], P('sp', 'tp')
The draws below stay inside these ranges and needn't reach their ends.
Inputs may be any that keep to these rules, and one draw needn't show every extreme that they name: `routes`: among the choices of one device's tokens no expert is named more than 96 times, a bound that some block reaches on some device; a token's choices differ.
All inputs are finite; a program needn't handle non-finite values.
Results may differ from the reference program's by a relative error of at most 0.0057.
Values may be sent and summed in bfloat16 or wider, within the bound.
No kernel may reach another device: no remote copies, remote signals or barrier semaphores. Data moves between devices by JAX's collectives and lax.ppermute only.
A program may use at most 128 MiB of HBM per device.

```python
import math
import jax
import jax.numpy as jnp
import numpy as np
from jax import lax

D = 2048
D_CH = 512
FF = 3584
KSIZE = 31
TOP = 2
GROUP = 2
TOK_DEV = 128
TOKENS = 1024
EXPERTS = 4
CAP = 96
N_SP = 8


def draw_normed(key, part):
    first_key, second_key, third_key = jax.random.split(key, 3)
    levels = jax.random.permutation(first_key, jnp.array([-0.7, 0.0, 0.7, 1.4], jnp.float32))
    spread = jax.random.uniform(second_key, (D_CH,), jnp.float32, -1.0, 1.0)
    channel_scale = jnp.exp(jnp.repeat(levels, D_CH // 4) + 0.3 * spread)
    base_values = jnp.clip(jax.random.normal(third_key, (TOKENS, D_CH), jnp.float32), -4.0, 4.0)
    return (base_values * channel_scale[None, :]).astype(jnp.bfloat16)


def strengthened(drawn, stream_key, source, target, parts, factor):
    owner, partner = [(jnp.arange(drawn.shape[dim]) // (drawn.shape[dim] // parts)).reshape([-1 if axis == dim else 1 for axis in range(drawn.ndim)]) for dim in (source, target)]
    chosen = jax.random.permutation(stream_key, parts)[partner]
    strong = (owner == chosen) | (owner == (partner + parts // 2) % parts)
    return jnp.where(strong, factor * drawn, drawn)


def level_of(key, shape, cuts, smallest, high):
    factor_of = 1.0
    for dim, blocks in cuts:
        heights = jax.random.uniform(jax.random.fold_in(jax.random.fold_in(key, 6), dim), (blocks,), jnp.float32, smallest / len(cuts), high / len(cuts))
        factor_of = factor_of * jnp.repeat(jnp.exp(heights), shape[dim] // blocks).reshape((-1,) + (1,) * (len(shape) - 1 - dim))
    return factor_of


def shared_out(stream_key, own, number, rows, count, top, bound, slope):
    order = jax.random.permutation(stream_key, count)
    heavy_load, common = portions_of(count, rows * top, bound, slope, True), portions_of(count, rows * top, bound, slope, False)
    places = jnp.arange(count)

    def named(tallies, offset_by):
        used = int((tallies > 0).sum())
        fixed = max(1, used // 4)
        passed = fixed + (places - fixed + offset_by * (used - fixed)) % max(1, count - fixed)
        return jnp.zeros((count,), jnp.int32).at[order[jnp.where(places < fixed, places, passed)]].set(jnp.asarray(tallies, jnp.int32))

    tallies = jnp.where(number % 4 == 0, named(heavy_load, number // 4), named(common, number - number // 4 - 1))
    mixed = jax.random.permutation(jax.random.fold_in(own, 3), count)
    giver, sink = mixed[0:count // 2 * 2:2], mixed[1:count // 2 * 2:2]
    margin = jnp.minimum(tallies[giver] - 1, bound - tallies[sink]) // 2
    margin = jnp.where((giver == order[0]) | (sink == order[0]) | (tallies[sink] == 0), 0, jnp.maximum(margin, 0))
    passed = jax.random.randint(jax.random.fold_in(own, 4), (count // 2,), 0, 1 << 20) % (margin + 1)
    tallies = tallies.at[giver].add(-passed).at[sink].add(passed)
    labels = jnp.searchsorted(jnp.cumsum(tallies), jnp.arange(rows * top), side="right").astype(jnp.int32)
    table = labels.reshape(top, rows).T
    table = table[jax.random.permutation(jax.random.fold_in(own, 1), rows)]
    offset_by = jax.random.randint(jax.random.fold_in(own, 2), (rows, 1), 0, top)
    return jnp.take_along_axis(table, (jnp.arange(top)[None, :] + offset_by) % top, axis=1)


def portions_of(count, total, reach, skew, full):
    weights = [(1 << 20) // math.isqrt(rank ** skew) + 1 for rank in range(1, count + 1)]
    largest = reach if full else min(reach, max(-(-total // count), total * weights[0] // sum(weights)))
    least = 1 if total - largest >= count - 1 else 0
    holding, surplus = [largest] + [least] * (count - 1), total - largest - least * (count - 1)
    while surplus > 0:
        free = [i for i in range(1, count) if holding[i] < largest] or [i for i in range(1, count) if holding[i] < reach]
        whole, remaining = sum([weights[i] for i in free]), surplus
        for i in free:
            extra = min(reach - holding[i], max(1, remaining * weights[i] // whole), surplus)
            holding[i] = holding[i] + extra
            surplus = surplus - extra
    return np.array(holding)


def scatter_about(key, extent, width, bound, pieces=(), kind=jnp.bfloat16):
    entries = width * jax.random.normal(key, extent, jnp.float32)
    if pieces:
        entries = entries * level_of(key, extent, pieces, -0.22, 0.18)
    return jnp.clip(entries, -bound, bound).astype(kind)


def noise_with(stream_key, extent, scale, limit, cuts, heavy, kind=jnp.bfloat16):
    values = scale * jax.random.normal(stream_key, extent, jnp.float32)
    if cuts:
        values = values * level_of(stream_key, extent, cuts, -0.22, 0.18)
    return jnp.clip(strengthened(values, jax.random.fold_in(stream_key, 3), *heavy), -limit, limit).astype(kind)


def setup_inputs(seed: int = 0) -> dict:
    seeds = jax.random.split(jax.random.key(seed), 15)
    hidden_state = scatter_about(seeds[0], (TOKENS, D), 1.0, 6.0, ((0, 8),))
    out_grad = noise_with(seeds[1], (TOKENS, D), 1.0, 8.0, ((0, 8),), (0, 1, 8, 2.0))
    routes_keys = jax.random.split(jax.random.fold_in(seeds[2], 1), TOKENS // TOK_DEV)
    routes_turns = jax.random.permutation(jax.random.fold_in(seeds[2], 3), TOKENS // TOK_DEV)
    routes = jax.vmap(lambda own, number: shared_out(jax.random.fold_in(seeds[2], 2), own, number, TOK_DEV, EXPERTS, TOP, CAP, 1))(routes_keys, routes_turns).reshape((TOKENS, TOP))
    route_weights = jnp.clip(0.25 + 0.75 * jax.random.uniform(seeds[3], (TOKENS, TOP), jnp.float32) ** level_of(seeds[3], (TOKENS, TOP), ((0, 8),), -0.2, 0.2), 0.25, 1.0)
    w_gate = scatter_about(seeds[4], (EXPERTS * GROUP, D, FF // GROUP), D ** -0.5, 0.125, ((0, 8), (2, 4)))
    w_up = scatter_about(seeds[5], (EXPERTS * GROUP, D, FF // GROUP), D ** -0.5, 0.125, ((0, 8), (2, 4)))
    w_down = scatter_about(seeds[6], (EXPERTS * GROUP, FF // GROUP, D), FF ** -0.5, 0.09375, ((0, 8), (1, 4)))
    value = scatter_about(seeds[7], (TOKENS, D_CH), 1.0, 6.0, ((0, 8), (1, 4)))
    gate_in = scatter_about(seeds[8], (TOKENS, D_CH), 1.0, 6.0, ((0, 8), (1, 4)))
    normed = draw_normed(jax.random.fold_in(seeds[14], 71), 0)
    inv_std = jnp.clip(jnp.exp(math.log(2.0) - 1.3862944 * jax.random.uniform(seeds[10], (TOKENS,), jnp.float32) ** level_of(seeds[10], (TOKENS,), ((0, 8),), -0.2, 0.2)), 0.5, 2.0)
    norm_gain = jnp.clip(1.0 + 0.18 * jax.random.normal(seeds[11], (D_CH,), jnp.float32), 0.1, 1.9)
    taps = scatter_about(seeds[12], (KSIZE, D_CH), 0.18, 1.0, ((1, 4),), jnp.float32)
    w_proj = scatter_about(seeds[13], (D, D_CH), D_CH ** -0.5, 0.25, ((1, 4),))
    return dict(hidden_state=hidden_state, out_grad=out_grad, routes=routes, route_weights=route_weights, w_gate=w_gate, w_up=w_up, w_down=w_down, value=value, gate_in=gate_in, normed=normed, inv_std=inv_std, norm_gain=norm_gain, taps=taps, w_proj=w_proj)


def expert_backward(in_rows, in_cots, gate_slice, up_slice, down_slice):
    pre_gate = jnp.dot(in_rows, gate_slice, preferred_element_type=jnp.float32)
    pre_up = jnp.dot(in_rows, up_slice, preferred_element_type=jnp.float32)
    gate_sig = jax.nn.sigmoid(pre_gate)
    silu_gate = pre_gate * gate_sig
    act_rows = (silu_gate * pre_up).astype(jnp.bfloat16)
    act_grad = lax.dot_general(in_cots, down_slice, (((1,), (1,)), ((), ())), preferred_element_type=jnp.float32)
    gate_grad = (act_grad * pre_up * gate_sig * (1.0 + pre_gate * (1.0 - gate_sig))).astype(jnp.bfloat16)
    up_grad = (act_grad * silu_gate).astype(jnp.bfloat16)
    down_grad = lax.dot_general(act_rows, in_cots, (((0,), (0,)), ((), ())), preferred_element_type=jnp.float32)
    gate_wgrad = lax.dot_general(in_rows, gate_grad, (((0,), (0,)), ((), ())), preferred_element_type=jnp.float32)
    up_wgrad = lax.dot_general(in_rows, up_grad, (((0,), (0,)), ((), ())), preferred_element_type=jnp.float32)
    row_grad = lax.dot_general(gate_grad, gate_slice, (((1,), (1,)), ((), ())), preferred_element_type=jnp.float32)
    row_grad = row_grad + lax.dot_general(up_grad, up_slice, (((1,), (1,)), ((), ())), preferred_element_type=jnp.float32)
    return gate_wgrad.astype(jnp.bfloat16), up_wgrad.astype(jnp.bfloat16), down_grad.astype(jnp.bfloat16), row_grad


def reference(hidden_state, out_grad, routes, route_weights, w_gate, w_up, w_down, value, gate_in, normed, inv_std, norm_gain, taps, w_proj):
    tokens, model_width = hidden_state.shape
    top_k = routes.shape[1]
    experts = N_SP // GROUP
    capacity = 3 * TOK_DEV * top_k // (2 * experts)
    per_dev = routes.reshape(N_SP, TOK_DEV * top_k).astype(jnp.int32)
    onehot = (per_dev[:, :, None] == jnp.arange(experts, dtype=jnp.int32)[None, None, :]).astype(jnp.int32)
    before = jnp.cumsum(onehot, axis=1) - onehot
    slot_index = jnp.sum(before * onehot, axis=2)
    source = jnp.arange(N_SP, dtype=jnp.int32)[:, None]
    slot_place = per_dev * (N_SP * capacity) + source * capacity + slot_index
    row_owner = source * TOK_DEV + jnp.arange(TOK_DEV * top_k, dtype=jnp.int32)[None, :] // top_k
    row_table = jnp.full((experts * N_SP * capacity,), tokens, jnp.int32)
    row_table = row_table.at[slot_place.reshape(-1)].set(row_owner.reshape(-1).astype(jnp.int32))
    row_table = row_table.reshape(experts, N_SP * capacity)
    row_scale = jnp.zeros((experts * N_SP * capacity,), jnp.float32)
    row_scale = row_scale.at[slot_place.reshape(-1)].set(route_weights.reshape(-1).astype(jnp.float32))
    row_scale = row_scale.reshape(experts, N_SP * capacity)
    zero_row = jnp.zeros((1, model_width), jnp.bfloat16)
    states = jnp.concatenate([hidden_state, zero_row], axis=0)
    cot_pad = jnp.concatenate([out_grad, zero_row], axis=0)

    def turn(row_total, slice_index):
        expert = (slice_index // GROUP).astype(jnp.int32)
        row_index = lax.dynamic_index_in_dim(row_table, expert, 0, False)
        scale_e = lax.dynamic_index_in_dim(row_scale, expert, 0, False)
        in_rows = jnp.take(states, row_index, axis=0)
        in_cots = (jnp.take(cot_pad, row_index, axis=0).astype(jnp.float32) * scale_e[:, None]).astype(jnp.bfloat16)
        gate_slice = lax.dynamic_index_in_dim(w_gate, slice_index, 0, False)
        up_slice = lax.dynamic_index_in_dim(w_up, slice_index, 0, False)
        down_slice = lax.dynamic_index_in_dim(w_down, slice_index, 0, False)
        gate_wgrad, up_wgrad, down_grad, row_grad = expert_backward(in_rows, in_cots, gate_slice, up_slice, down_slice)
        row_total = row_total.at[row_index].add(row_grad)
        return row_total, (gate_wgrad, up_wgrad, down_grad)

    row_total, weight_grads = lax.scan(turn, jnp.zeros((tokens + 1, model_width), jnp.float32), jnp.arange(experts * GROUP, dtype=jnp.int32))
    moe_grad = row_total[:tokens]
    stream_grad = (out_grad.astype(jnp.float32) + moe_grad).astype(jnp.bfloat16)
    proj_in = jnp.dot(stream_grad, w_proj, preferred_element_type=jnp.float32)
    saved_norm = normed.astype(jnp.float32)
    pre_act = saved_norm * norm_gain[None, :]
    act_sig = jax.nn.sigmoid(pre_act)
    silu_grad = proj_in * act_sig * (1.0 + pre_act * (1.0 - act_sig))
    norm_grad = silu_grad * norm_gain[None, :]
    mean_one = jnp.mean(norm_grad, axis=1, keepdims=True)
    mean_two = jnp.mean(norm_grad * saved_norm, axis=1, keepdims=True)
    conv_grad = inv_std[:, None] * (norm_grad - mean_one - saved_norm * mean_two)
    channels = conv_grad.shape[1]
    extended = jnp.concatenate([conv_grad, jnp.zeros((KSIZE - 1, channels), jnp.float32)], axis=0)
    glu_grad = taps[0][None, :] * extended[0:tokens]
    for tap_index in range(1, KSIZE):
        glu_grad = glu_grad + taps[tap_index][None, :] * extended[tap_index:tap_index + tokens]
    input_sig = jax.nn.sigmoid(gate_in.astype(jnp.float32))
    value_grad = (glu_grad * input_sig).astype(jnp.bfloat16)
    gate_in_grad = (glu_grad * value.astype(jnp.float32) * input_sig * (1.0 - input_sig)).astype(jnp.bfloat16)
    proj_act = (pre_act * act_sig).astype(jnp.bfloat16)
    proj_grad = lax.dot_general(stream_grad, proj_act, (((0,), (0,)), ((), ())), preferred_element_type=jnp.float32)
    return weight_grads[0], weight_grads[1], weight_grads[2], stream_grad, proj_grad, value_grad, gate_in_grad
```

```python
import jax
import jax.numpy as jnp
from jax import lax
from jax.sharding import PartitionSpec as P

D_CH = 512
KSIZE = 31
GROUP = 2


def passed_along(value, axis, by):
    peers = lax.axis_size(axis)
    pairs = [(i, i + by) for i in range(peers) if 0 <= i + by < peers]
    return lax.ppermute(value, axis, pairs)


def to_expert(value, by):
    ways = lax.axis_size("sp")
    experts = ways // GROUP
    pairs = [(i, ((i // GROUP + by) % experts) * GROUP + i % GROUP) for i in range(ways)]
    return lax.ppermute(value, "sp", pairs)


def to_mate(value):
    return lax.ppermute(value, "sp", [(i, i ^ 1) for i in range(lax.axis_size("sp"))])


def to_part(value, bit):
    return lax.ppermute(value, "tp", [(i, i ^ bit) for i in range(lax.axis_size("tp"))])


def dot_t(left, right, left_dim, right_dim):
    return lax.dot_general(
        left, right, (((left_dim,), (right_dim,)), ((), ())), preferred_element_type=jnp.float32
    )


def slot_table(routes, route_weights, my_expert, experts, capacity):
    tok_rows = routes.shape[0]
    turned = (routes - my_expert) % experts
    named = turned.T[None, :, :] == jnp.arange(experts, dtype=jnp.int32)[:, None, None]
    member = jnp.any(named, axis=1)
    scale = jnp.sum(jnp.where(named, route_weights.T[None, :, :], 0.0), axis=1)
    earlier = (
        jnp.arange(tok_rows)[:, None] < jnp.arange(tok_rows)[None, :]
    ).astype(jnp.bfloat16)
    rank = jnp.dot(member.astype(jnp.bfloat16), earlier, preferred_element_type=jnp.float32)
    rank = jnp.where(member, rank.astype(jnp.int32), -1)
    chosen = rank[:, None, :] == jnp.arange(capacity, dtype=jnp.int32)[None, :, None]
    row_scale = jnp.sum(jnp.where(chosen, scale[:, None, :], 0.0), axis=2)
    return (
        chosen.astype(jnp.bfloat16).reshape(experts * capacity, tok_rows),
        row_scale.reshape(experts * capacity, 1),
    )


def dispatched(packed, experts):
    capacity = packed.shape[0] // experts
    blocks = [packed[:capacity]]
    for by in range(1, experts):
        blocks.append(to_expert(packed[by * capacity : (by + 1) * capacity], by))
    mine = jnp.concatenate(blocks, axis=0)
    half = mine.shape[0] // 2
    mate = to_mate(mine)
    far = to_part(mine, 2)
    diagonal = [to_part(mate[:half], 2), to_mate(far[half:])]
    own_part = jnp.concatenate([mine, mate], axis=0)
    far_part = jnp.concatenate([far] + diagonal, axis=0)
    return [own_part, to_part(own_part, 1), far_part, to_part(far_part, 1)]


def returned(parts, experts):
    rows = parts[0].shape[0]
    half = rows // 4
    mid = rows // 2
    narrow = lambda v: v.astype(jnp.bfloat16)
    wide = lambda v: v.astype(jnp.float32)
    own = parts[0] + wide(to_part(narrow(parts[1]), 1))
    far = parts[2] + wide(to_part(narrow(parts[3]), 1))
    low_diag = wide(to_part(narrow(far[mid : mid + half]), 2))
    high_diag = wide(to_mate(narrow(far[mid + half :])))
    far_low = wide(to_part(narrow(far[:half]), 2))
    mate_high = wide(to_mate(narrow(own[mid + half :])))
    far_high = wide(to_part(narrow(far[half:mid] + high_diag), 2))
    mate_low = wide(to_mate(narrow(own[mid : mid + half] + low_diag)))
    low = narrow(own[:half] + far_low + mate_low)
    high = narrow(own[half:mid] + far_high + mate_high)
    mine = jnp.concatenate([low, high], axis=0)
    capacity = mid // experts
    blocks = [mine[:capacity]]
    for by in range(1, experts):
        blocks.append(to_expert(mine[by * capacity : (by + 1) * capacity], -by))
    return jnp.concatenate(blocks, axis=0)


def on_device(
    hidden_state,
    out_grad,
    routes,
    route_weights,
    w_gate,
    w_up,
    w_down,
    value,
    gate_in,
    normed,
    inv_std,
    norm_gain,
    taps,
    w_proj,
):
    tok_rows, model_width = hidden_state.shape
    top_k = routes.shape[1]
    sp_ways = lax.axis_size("sp")
    tp_parts = lax.axis_size("tp")
    experts = sp_ways // GROUP
    capacity = 3 * tok_rows * top_k // (2 * experts)
    quarter = model_width // tp_parts
    part = lax.axis_index("tp")
    my_expert = lax.axis_index("sp") // GROUP
    my_slice = lax.axis_index("sp") % GROUP
    turned = [part ^ i for i in range(tp_parts)]
    pick, row_scale = slot_table(routes, route_weights, my_expert, experts, capacity)
    cot_part = lax.dynamic_slice_in_dim(out_grad, part * quarter, quarter, 1)
    part_states = lax.dynamic_slice_in_dim(hidden_state, part * quarter, quarter, 1)
    sent_rows = jnp.dot(pick, part_states, preferred_element_type=jnp.float32)
    sent_cots = jnp.dot(pick, cot_part, preferred_element_type=jnp.float32)
    rows = dispatched(sent_rows.astype(jnp.bfloat16), experts)
    cots = dispatched((sent_cots * row_scale).astype(jnp.bfloat16), experts)

    gates = [lax.dynamic_slice_in_dim(w_gate[0], i * quarter, quarter, 0) for i in turned]
    ups = [lax.dynamic_slice_in_dim(w_up[0], i * quarter, quarter, 0) for i in turned]
    downs = [lax.dynamic_slice_in_dim(w_down[0], i * quarter, quarter, 1) for i in turned]
    order = [0, 2, 1, 3]
    pre_gate = sum(dot_t(rows[i], gates[i], 1, 0) for i in order)
    pre_up = sum(dot_t(rows[i], ups[i], 1, 0) for i in order)
    act_grad = sum(dot_t(cots[i], downs[i], 1, 1) for i in order)
    gate_sig = jax.nn.sigmoid(pre_gate)
    silu_gate = pre_gate * gate_sig
    act_rows = (silu_gate * pre_up).astype(jnp.bfloat16)
    gate_grad = (act_grad * pre_up * gate_sig * (1.0 + pre_gate * (1.0 - gate_sig))).astype(
        jnp.bfloat16
    )
    up_grad = (act_grad * silu_gate).astype(jnp.bfloat16)
    row_parts = [dot_t(gate_grad, gates[i], 1, 1) + dot_t(up_grad, ups[i], 1, 1) for i in range(4)]
    back_rows = returned(row_parts, experts)

    gate_wgrad = jnp.zeros(w_gate.shape[1:], jnp.bfloat16)
    up_wgrad = jnp.zeros(w_up.shape[1:], jnp.bfloat16)
    down_grad = jnp.zeros(w_down.shape[1:], jnp.bfloat16)
    for i in range(tp_parts):
        at = turned[i] * quarter
        gate_wgrad = lax.dynamic_update_slice_in_dim(
            gate_wgrad, dot_t(rows[i], gate_grad, 0, 0).astype(jnp.bfloat16), at, 0
        )
        up_wgrad = lax.dynamic_update_slice_in_dim(
            up_wgrad, dot_t(rows[i], up_grad, 0, 0).astype(jnp.bfloat16), at, 0
        )
        down_grad = lax.dynamic_update_slice_in_dim(
            down_grad, dot_t(act_rows, cots[i], 0, 0).astype(jnp.bfloat16), at, 1
        )

    moe_part = dot_t(pick, back_rows, 0, 0)
    stream_part = (cot_part.astype(jnp.float32) + moe_part).astype(jnp.bfloat16)
    stream_full = lax.all_gather(stream_part, "tp", axis=1, tiled=True)
    proj_in = jnp.dot(stream_full, w_proj, preferred_element_type=jnp.float32)
    saved_norm = normed.astype(jnp.float32)
    pre_act = saved_norm * norm_gain[None, :]
    act_sig = jax.nn.sigmoid(pre_act)
    silu_grad = proj_in * act_sig * (1.0 + pre_act * (1.0 - act_sig))
    norm_grad = silu_grad * norm_gain[None, :]
    sums = jnp.stack([jnp.sum(norm_grad, axis=1), jnp.sum(norm_grad * saved_norm, axis=1)])
    sums = sums + sum(to_part(sums, i) for i in range(1, tp_parts))
    mean_one = sums[0] / D_CH
    mean_two = sums[1] / D_CH
    conv_grad = inv_std[:, None] * (norm_grad - mean_one[:, None] - saved_norm * mean_two[:, None])
    tail_rows = passed_along(conv_grad[: KSIZE - 1], "sp", -1)
    extended = jnp.concatenate([conv_grad, tail_rows], axis=0)
    glu_grad = taps[0][None, :] * extended[0:tok_rows]
    for tap_index in range(1, KSIZE):
        glu_grad = glu_grad + taps[tap_index][None, :] * extended[tap_index : tap_index + tok_rows]
    input_sig = jax.nn.sigmoid(gate_in.astype(jnp.float32))
    value_grad = (glu_grad * input_sig).astype(jnp.bfloat16)
    gate_in_grad = (glu_grad * value.astype(jnp.float32) * input_sig * (1.0 - input_sig)).astype(
        jnp.bfloat16
    )
    proj_act = (pre_act * act_sig).astype(jnp.bfloat16)
    partial = dot_t(stream_full, proj_act, 0, 0)
    channels = partial.shape[1]
    piece = model_width // sp_ways
    partial = partial.reshape(experts, GROUP, piece, channels)
    kept = lax.dynamic_index_in_dim(partial, my_slice, 1, False)
    other = lax.dynamic_index_in_dim(partial, (my_slice + 1) % GROUP, 1, False)
    kept = kept + to_mate(other.astype(jnp.bfloat16)).astype(jnp.float32)
    proj_grad = lax.dynamic_index_in_dim(kept, my_expert, 0, False)
    for by in range(1, experts):
        block = lax.dynamic_index_in_dim(kept, (my_expert + by) % experts, 0, False)
        proj_grad = proj_grad + to_expert(block.astype(jnp.bfloat16), by).astype(jnp.float32)
    return (
        gate_wgrad[None],
        up_wgrad[None],
        down_grad[None],
        stream_part,
        proj_grad,
        value_grad,
        gate_in_grad,
    )


def solution(mesh):
    in_specs = (
        P("sp", None),
        P("sp", None),
        P("sp", None),
        P("sp", None),
        P("sp", None, "tp"),
        P("sp", None, "tp"),
        P("sp", "tp", None),
        P("sp", "tp"),
        P("sp", "tp"),
        P("sp", "tp"),
        P("sp"),
        P("tp"),
        P(None, "tp"),
        P(None, "tp"),
    )
    out_specs = (
        P("sp", None, "tp"),
        P("sp", None, "tp"),
        P("sp", "tp", None),
        P("sp", "tp"),
        P("sp", "tp"),
        P("sp", "tp"),
        P("sp", "tp"),
    )
    return jax.shard_map(
        on_device, mesh=mesh, in_specs=in_specs, out_specs=out_specs, check_vma=False
    )
```
